512 devices in a mesh: sp: 64 (over z, y), tp: 8 (over x, core).
Axes of the slice: x: 4, y: 4, z: 16, core: 2. Of those that a mesh axis runs over, the one named last changes fastest.
Arguments:
- tokens: bfloat16 [16384, 2048], P('sp', 'tp'), may hold values from -6 to 6
- outer_gate: bfloat16 [2048, 1024], P(None, 'tp'), may hold values from -0.125 to 0.125
- inner_gate: bfloat16 [2048, 1024], P(None, 'tp'), may hold values from -0.125 to 0.125
- conv_input: bfloat16 [2048, 1024], P(None, 'tp'), may hold values from -0.125 to 0.125
- conv_taps: bfloat16 [3, 1024], P(None, 'tp'), may hold values from -3.5 to 3.5
- query_down: bfloat16 [2048, 512], P(None, 'tp'), may hold values from -0.125 to 0.125
- latent_down: bfloat16 [2048, 256], P(None, 'tp'), may hold values from -0.125 to 0.125
- rotary_down: bfloat16 [2048, 32], replicated, may hold values from -5.303301 to 5.303301
- query_gain: float32 [512], replicated, may hold values from 0.1 to 1.9
- latent_gain: float32 [256], replicated, may hold values from 0.1 to 1.9
- query_up: bfloat16 [512, 1536], P(None, 'tp'), may hold values from -0.52734375 to 0.52734375
- latent_up: bfloat16 [256, 2048], P(None, 'tp'), may hold values from -0.75 to 0.75
- conv_project: bfloat16 [1024, 2048], P('tp'), may hold values from -0.1875 to 0.1875
- attend_project: bfloat16 [1024, 2048], P('tp'), may hold values from -0.1875 to 0.1875
Outputs:
- mixed: bfloat16 [16384, 2048], P(('sp', 'tp'))
The draws below stay inside these ranges and needn't reach their ends.
All inputs are finite; a program needn't handle non-finite values.
Results may differ from the reference program's by a relative error of at most 0.035.
Values may be sent and summed in bfloat16 or wider, within the bound.
No kernel may reach another device: no remote copies, remote signals or barrier semaphores. Data moves between devices by JAX's collectives and lax.ppermute only.
A program may use at most 128 MiB of HBM per device.

```python
import math
import jax
import jax.numpy as jnp
from jax import lax

D = 2048
CW = 1024
HEADS = 16
QR = 512
KVR = 256
NOPE = 64
ROPE = 32
VDIM = 64
KSIZE = 3
TOKENS = 16384
N_TP = 8


def draw_rotary_down(key, part):
    base = jnp.clip(jax.random.normal(key, (D, ROPE), jnp.float32), -6.0, 6.0) * D ** (-0.5)
    return base.astype(jnp.bfloat16)


def steps_of(own_key, dims, shards, smallest, high):
    def one(dim, parts):
        draws = jax.random.uniform(jax.random.fold_in(jax.random.fold_in(own_key, 6), dim), (parts,), jnp.float32, smallest / len(shards), high / len(shards))
        return jnp.repeat(jnp.exp(draws), dims[dim] // parts).reshape((-1,) + (1,) * (len(dims) - dim - 1))

    loudness = one(*shards[0])
    for cut in shards[1:]:
        loudness = loudness * one(*cut)
    return loudness


def noise(stream_key, dims, deviation, most, shards=(), held_as=jnp.bfloat16):
    values = deviation * jax.random.normal(stream_key, dims, jnp.float32)
    if shards:
        values = values * steps_of(stream_key, dims, shards, -0.22, 0.18)
    return jnp.clip(values, -most, most).astype(held_as)


def setup_inputs(seed: int = 0) -> dict:
    keys = jax.random.split(jax.random.key(seed), 15)
    tokens = noise(keys[0], (TOKENS, D), 1.0, 6.0, ((0, 64), (1, 8)))
    outer_gate = noise(keys[1], (D, CW), D ** -0.5, 0.125, ((1, 8),))
    inner_gate = noise(keys[2], (D, CW), D ** -0.5, 0.125, ((1, 8),))
    conv_input = noise(keys[3], (D, CW), D ** -0.5, 0.125, ((1, 8),))
    conv_taps = noise(keys[4], (KSIZE, CW), KSIZE ** -0.5, 3.5, ((1, 8),))
    query_down = noise(keys[5], (D, QR), D ** -0.5, 0.125, ((1, 8),))
    latent_down = noise(keys[6], (D, KVR), D ** -0.5, 0.125, ((1, 8),))
    rotary_down = draw_rotary_down(jax.random.fold_in(keys[14], 71), 0)
    query_gain = jnp.clip(1.0 + 0.18 * jax.random.normal(keys[8], (QR,), jnp.float32), 0.1, 1.9)
    latent_gain = jnp.clip(1.0 + 0.18 * jax.random.normal(keys[9], (KVR,), jnp.float32), 0.1, 1.9)
    query_up = noise(keys[10], (QR, HEADS * (NOPE + ROPE)), (2.0 / QR ** 0.5), 0.52734375, ((1, 8),))
    latent_up = noise(keys[11], (KVR, HEADS * (NOPE + VDIM)), (2.0 / KVR ** 0.5), 0.75, ((1, 8),))
    conv_project = noise(keys[12], (CW, D), CW ** -0.5, 0.1875, ((0, 8),))
    attend_project = noise(keys[13], (HEADS * VDIM, D), (HEADS * VDIM) ** -0.5, 0.1875, ((0, 8),))
    return {"tokens": tokens, "outer_gate": outer_gate, "inner_gate": inner_gate, "conv_input": conv_input, "conv_taps": conv_taps, "query_down": query_down, "latent_down": latent_down, "rotary_down": rotary_down, "query_gain": query_gain, "latent_gain": latent_gain, "query_up": query_up, "latent_up": latent_up, "conv_project": conv_project, "attend_project": attend_project}


neg_fill = -1e+30
rotary_base = 10000.0
norm_epsilon = 1e-06

def matmul(left, right):
    return jnp.dot(left, right, preferred_element_type=jnp.float32)

def rotate(values, positions):
    half = values.shape[-1] // 2
    inverse = rotary_base ** (-(jnp.arange(half, dtype=jnp.float32) * 2.0 / (2 * half)))
    angle = positions[:, None] * inverse[None, :]
    if values.ndim == 3:
        angle = angle[:, None, :]
    cosine = jnp.cos(angle)
    sine = jnp.sin(angle)
    first = values[..., :half]
    second = values[..., half:]
    return jnp.concatenate([first * cosine - second * sine, first * sine + second * cosine], -1)

def rms_scale(latent, gain):
    values = lax.optimization_barrier(latent).astype(jnp.float32)
    factor = lax.rsqrt(lax.optimization_barrier(jnp.mean(values * values, -1, keepdims=True)) + norm_epsilon)
    return (values * factor * gain).astype(jnp.bfloat16)

def reference(tokens, outer_gate, inner_gate, conv_input, conv_taps, query_down, latent_down, rotary_down, query_gain, latent_gain, query_up, latent_up, conv_project, attend_project):
    length = tokens.shape[0]
    outer = matmul(tokens, outer_gate)
    inner = matmul(tokens, inner_gate)
    signal = matmul(tokens, conv_input)
    gated = lax.optimization_barrier((inner * signal).astype(jnp.bfloat16)).astype(jnp.float32)
    padded = jnp.pad(gated, ((KSIZE - 1, 0), (0, 0)))
    taps = conv_taps.astype(jnp.float32)
    filtered = padded[0:length] * taps[0]
    for index in range(1, KSIZE):
        filtered = filtered + padded[index:index + length] * taps[index]
    conv_result = (outer * filtered).astype(jnp.bfloat16)
    positions = jnp.arange(length, dtype=jnp.float32)
    query_norm = rms_scale(matmul(tokens, query_down).astype(jnp.bfloat16), query_gain)
    latent_norm = rms_scale(matmul(tokens, latent_down).astype(jnp.bfloat16), latent_gain)
    rotary_key = rotate(matmul(tokens, rotary_down), positions).astype(jnp.bfloat16)
    query_full = matmul(query_norm, query_up).reshape(length, HEADS, NOPE + ROPE)
    query_plain = query_full[..., :NOPE].astype(jnp.bfloat16).astype(jnp.float32)
    query_rot = rotate(query_full[..., NOPE:], positions).astype(jnp.bfloat16).astype(jnp.float32)
    expanded = matmul(latent_norm, latent_up).astype(jnp.bfloat16).reshape(length, HEADS, NOPE + VDIM)
    key_plain = expanded[..., :NOPE].astype(jnp.float32)
    values = expanded[..., NOPE:].astype(jnp.float32)
    key_rot = rotary_key.astype(jnp.float32)
    scale = (NOPE + ROPE) ** (-0.5)
    block = math.gcd(length, 256)
    key_index = jnp.arange(length)

    def one_block(number):
        first = (number * block).astype(jnp.int32)
        plain = lax.dynamic_slice_in_dim(query_plain, first, block, 0)
        turned = lax.dynamic_slice_in_dim(query_rot, first, block, 0)
        scores = jnp.einsum('qhd,khd->hqk', plain, key_plain) + jnp.einsum('qhr,kr->hqk', turned, key_rot)
        scores = scores * scale
        query_index = first + jnp.arange(block)
        visible = key_index[None, :] <= query_index[:, None]
        scores = jnp.where(visible[None], scores, neg_fill)
        rowmax = lax.optimization_barrier(jnp.max(scores, -1, keepdims=True))
        weight = jnp.exp(scores - rowmax)
        total = lax.optimization_barrier(jnp.sum(weight, -1))
        rounded = weight.astype(jnp.bfloat16).astype(jnp.float32)
        summed = jnp.einsum('hqk,khd->qhd', rounded, values)
        return (summed / total.T[:, :, None]).astype(jnp.bfloat16)
    attended = lax.map(one_block, jnp.arange(length // block, dtype=jnp.int32))
    attended = attended.reshape(length, HEADS * VDIM)
    conv_share = CW // N_TP
    head_share = HEADS * VDIM // N_TP
    result = jnp.zeros((length, D), jnp.float32)
    for group in range(N_TP):
        partial_value = matmul(conv_result[:, group * conv_share:(group + 1) * conv_share], conv_project[group * conv_share:(group + 1) * conv_share])
        partial_value = partial_value + matmul(attended[:, group * head_share:(group + 1) * head_share], attend_project[group * head_share:(group + 1) * head_share])
        result = result + lax.optimization_barrier(partial_value.astype(jnp.bfloat16)).astype(jnp.float32)
    return result.astype(jnp.bfloat16)
```

```python
import math

import jax
import jax.numpy as jnp
from jax import lax
from jax.experimental import pallas as pl
from jax.experimental.pallas import tpu as pltpu
from jax.sharding import Mesh
from jax.sharding import PartitionSpec as P

NOPE = 64
ROPE = 32
VDIM = 64
SP = ("sp_0", "sp_1")
SP_TP = ("sp_0", "sp_1", "tp")
NZ = 16
NY = 4
ROWS = 256
HEADS = 2
CHUNK = 4
STATS = 16
Y_SHIFTS = (0, 1, 3, 2)
X_SHIFTS = (0, 1, 3, 2)

neg_fill = -1e30
rotary_base = 10000.0
norm_epsilon = 1e-06
bf16 = jnp.bfloat16
f32 = jnp.float32
VMEM = pl.BlockSpec(memory_space=pltpu.VMEM)
SMEM = pl.BlockSpec(memory_space=pltpu.SMEM)


def params():
    return pltpu.CompilerParams(vmem_limit_bytes=48 * 1024 * 1024)


def cost(flops):
    return pl.CostEstimate(flops=flops, bytes_accessed=4 * 1024 * 1024, transcendentals=0)


def dot(a, b):
    return jnp.dot(a, b, preferred_element_type=f32)


def latents_kernel(tok, wl, wr, wq, cos, sin, kr_out, q_out):
    groups, rows, width = tok.shape
    lat = jnp.zeros((rows, wl.shape[1]), f32)
    rot = jnp.zeros((rows, wr.shape[1]), f32)
    qry = jnp.zeros((rows, wq.shape[1]), f32)
    for g in range(groups):
        piece = tok[g]
        span = pl.ds(g * width, width)
        lat = lat + dot(piece, wl[span, :])
        rot = rot + dot(piece, wr[span, :])
        qry = qry + dot(piece, wq[span, :])
    both = jnp.concatenate([lat, rot, qry], 1).T
    half = ROPE // 2
    a = both[32 : 32 + half]
    b = both[32 + half : 64]
    c = cos[...]
    s = sin[...]
    kr_out[...] = jnp.concatenate([both[:32], a * c - b * s, a * s + b * c], 0).astype(bf16)
    q_out[...] = both[64:].astype(bf16)


def gates_kernel(tok, wo, wi, ws, outer_out, gated_out):
    groups, rows, width = tok.shape
    outer = jnp.zeros((rows, wo.shape[1]), f32)
    inner = outer
    signal = outer
    for g in range(groups):
        piece = tok[g]
        span = pl.ds(g * width, width)
        outer = outer + dot(piece, wo[span, :])
        inner = inner + dot(piece, wi[span, :])
        signal = signal + dot(piece, ws[span, :])
    outer_out[...] = outer
    gated_out[...] = (inner * signal).astype(bf16)


def normed(lat, gain):
    factor = lax.rsqrt(jnp.mean(lat * lat, 0, keepdims=True) + norm_epsilon)
    return (lat * factor * gain).astype(bf16)


def attention_kernel(where, *refs):
    lats = refs[:8]
    gathered, wq, wk, gq, gk, cos, sin, out, q_s, k_s, v_s, acc_s, m_s = refs[8:]
    z = where[0]
    y = where[1]
    per = NOPE + ROPE
    half = ROPE // 2
    scale = per ** (-0.5) * math.log2(math.e)
    for j in range(NY):
        base = NZ * 32 + 64 * j
        lat = jnp.concatenate([a[base : base + 64, :] for a in lats], 0).astype(f32)
        full = dot(wq[...], normed(lat, gq[...])) * scale
        c = cos[:, ROWS * j : ROWS * (j + 1)]
        s = sin[:, ROWS * j : ROWS * (j + 1)]
        for h in range(HEADS):
            at = per * h
            a = full[at + NOPE : at + NOPE + half]
            b = full[at + NOPE + half : at + per]
            q_s[h, j] = jnp.concatenate(
                [full[at : at + NOPE], a * c - b * s, a * s + b * c], 0
            ).astype(bf16)
            m_s[h, j] = jnp.full((8, ROWS), neg_fill, f32)
            acc_s[h, j] = jnp.zeros((VDIM + 16, ROWS), f32)
    for h in range(HEADS):
        v_s[h, VDIM:, :] = jnp.ones((16, CHUNK * ROWS), bf16)

    def chunk(number, masked):
        for b in range(CHUNK):
            zz = number * CHUNK + b
            start = pl.multiple_of(zz * 32, 32)
            lat = jnp.concatenate([a[pl.ds(start, 32), :] for a in lats], 0).astype(f32)
            full = dot(wk[...], normed(lat, gk[...])).astype(bf16)
            rot = gathered[zz, 32:64, :].astype(f32)
            for h in range(HEADS):
                at = (NOPE + VDIM) * h
                tall = jnp.concatenate([full[at : at + NOPE].astype(f32), rot], 0)
                k_s[h, ROWS * b : ROWS * (b + 1), :] = tall.T.astype(bf16)
                v_s[h, :VDIM, ROWS * b : ROWS * (b + 1)] = full[at + NOPE : at + NOPE + VDIM]
        for h in range(HEADS):
            for j in range(NY):
                scores = dot(k_s[h], q_s[h, j])
                if masked:
                    key = lax.broadcasted_iota(jnp.int32, (CHUNK * ROWS, ROWS), 0)
                    col = lax.broadcasted_iota(jnp.int32, (CHUNK * ROWS, ROWS), 1)
                    yq = lax.rem(y + NY - Y_SHIFTS[j], NY)
                    ahead = (z - number * CHUNK) * (NY * ROWS) + (yq - y) * ROWS
                    block = lax.shift_right_logical(key, 8)
                    scores = jnp.where(
                        key + block * (NY * ROWS - ROWS) - col <= ahead, scores, neg_fill
                    )
                old = m_s[h, j, 0:1, :]
                best = jnp.maximum(old, jnp.max(scores, 0, keepdims=True))
                weight = jnp.exp2(scores - best).astype(bf16)
                acc_s[h, j] = acc_s[h, j] * jnp.exp2(old - best) + dot(v_s[h], weight)
                m_s[h, j, 0:1, :] = best

    last = z // CHUNK

    def step(number, carry):
        chunk(number, False)
        return carry

    lax.fori_loop(0, last, step, 0)
    chunk(last, True)
    row = lax.broadcasted_iota(jnp.int32, (STATS, ROWS), 0)
    for j in range(NY):
        yq = lax.rem(y + NY - Y_SHIFTS[j], NY)
        stats = jnp.zeros((STATS, ROWS), f32)
        for h in range(HEADS):
            acc = acc_s[h, j]
            total = acc[VDIM : VDIM + 1]
            out[yq, VDIM * h : VDIM * (h + 1), :] = (acc[:VDIM] / total).astype(bf16)
            rest = m_s[h, j, 0:1, :] + jnp.log2(total)
            for part in range(3):
                piece = rest.astype(bf16).astype(f32)
                stats = jnp.where(row == 3 * h + part, piece, stats)
                rest = rest - piece
        out[yq, HEADS * VDIM :, :] = stats.astype(bf16)


def project_kernel(parts, outer, gated, rim, taps, wc, wa, out):
    rows, width = gated.shape
    mixed = []
    for h in range(HEADS):
        at = HEADS * VDIM
        logs = []
        for p in range(NY):
            stat = parts[p, at : at + STATS, :].astype(f32)
            logs.append(stat[3 * h : 3 * h + 1] + stat[3 * h + 1 : 3 * h + 2] + stat[3 * h + 2 : 3 * h + 3])
        best = jnp.maximum(jnp.maximum(logs[0], logs[1]), jnp.maximum(logs[2], logs[3]))
        total = jnp.zeros_like(best)
        summed = jnp.zeros((VDIM, rows), f32)
        for p in range(NY):
            weight = jnp.exp2(logs[p] - best)
            total = total + weight
            summed = summed + parts[p, VDIM * h : VDIM * (h + 1), :].astype(f32) * weight
        mixed.append(summed / total)
    attended = jnp.concatenate(mixed, 0).T.astype(bf16)
    here = gated[...].astype(f32)
    before = rim[...].astype(f32)
    row = lax.broadcasted_iota(jnp.int32, (rows, width), 0)
    one = jnp.where(row == 0, before[1:2], pltpu.roll(here, 1, 0))
    two = pltpu.roll(here, 2, 0)
    two = jnp.where(row == 0, before[0:1], jnp.where(row == 1, before[1:2], two))
    tap = taps[...].astype(f32)
    filtered = two * tap[0:1] + one * tap[1:2] + here * tap[2:3]
    conv = (outer[...] * filtered).astype(bf16)
    both = jnp.concatenate([conv, attended], 1)
    weights = jnp.concatenate([wc[...], wa[...]], 0)
    out[...] = dot(both, weights).astype(bf16)


def call(kernel, outs, flops, scratch=(), scalars=0):
    def run(*arrays):
        return pl.pallas_call(
            kernel,
            out_shape=outs,
            in_specs=[SMEM] * scalars + [VMEM] * (len(arrays) - scalars),
            out_specs=jax.tree.map(lambda _: VMEM, outs),
            scratch_shapes=list(scratch),
            compiler_params=params(),
            cost_estimate=cost(flops),
        )(*arrays)

    return run


def along_x(value, by):
    return lax.ppermute(value, "tp", [(i, (i + 2 * by) % 8) for i in range(8)])


def to_partner(value):
    return lax.ppermute(value, "tp", [(i, i ^ 1) for i in range(8)])


def along_y(value, by):
    return lax.ppermute(value, "sp_1", [(i, (i + by) % NY) for i in range(NY)])


def local(
    tokens,
    outer_gate,
    inner_gate,
    conv_input,
    conv_taps,
    query_down,
    latent_down,
    rotary_down,
    query_gain,
    latent_gain,
    query_up,
    latent_up,
    conv_project,
    attend_project,
):
    rows = tokens.shape[0]
    groups = lax.axis_size("tp")
    z = lax.axis_index("sp_0")
    y = lax.axis_index("sp_1")
    tp = lax.axis_index("tp")
    shapes = jax.ShapeDtypeStruct
    everyone = jnp.broadcast_to(tokens[None], (groups, *tokens.shape))
    pieces = lax.all_to_all(everyone, "tp", 0, 0, tiled=True)

    y_order = (y - jnp.array(Y_SHIFTS, jnp.int32)) % NY
    starts = (z * NY + y_order) * rows
    positions = (starts[:, None] + jnp.arange(rows, dtype=jnp.int32)[None]).reshape(-1).astype(f32)
    half = ROPE // 2
    inverse = rotary_base ** (-(jnp.arange(half, dtype=f32) * 2.0 / (2 * half)))
    angle = inverse[:, None] * positions[None, :]
    cosine = jnp.cos(angle)
    sine = jnp.sin(angle)
    x_order = (tp // 2 - jnp.array(X_SHIFTS, jnp.int32)) % 4
    order = jnp.concatenate([x_order * 2 + tp % 2, x_order * 2 + 1 - tp % 2])
    wq = jnp.take(query_up.reshape(8, 64, -1), order, axis=0).reshape(512, -1).T
    wk = jnp.take(latent_up.reshape(8, 32, -1), order, axis=0).reshape(256, -1).T
    gq = jnp.take(query_gain.reshape(8, 64), order, axis=0).reshape(512, 1)
    gk = jnp.take(latent_gain.reshape(8, 32), order, axis=0).reshape(256, 1)

    own_kr, own_q = call(
        latents_kernel, (shapes((64, rows), bf16), shapes((64, rows), bf16)), 2 * 256 * 2048 * 128
    )(pieces, latent_down, rotary_down, query_down, cosine[:, :rows], sine[:, :rows])
    queries = [own_q] + [along_y(own_q, by) for by in Y_SHIFTS[1:]]
    gathered = lax.all_gather(own_kr, "sp_0")
    mine = jnp.concatenate([gathered[:, :32].reshape(NZ * 32, rows), *queries], 0)
    held = [mine] + [along_x(mine, by) for by in X_SHIFTS[1:]]
    held = held + [to_partner(value) for value in held]

    outer, gated = call(
        gates_kernel, (shapes((rows, 128), f32), shapes((rows, 128), bf16)), 2 * 256 * 2048 * 384
    )(pieces, outer_gate, inner_gate, conv_input)
    length = lax.axis_size(SP)
    rim = lax.ppermute(gated[rows - 2 :], SP, [(i, i + 1) for i in range(length - 1)])

    parts = call(
        attention_kernel,
        shapes((NY, HEADS * VDIM + STATS, rows), bf16),
        2 * 1024 * 4096 * 512,
        (
            pltpu.VMEM((HEADS, NY, NOPE + ROPE, rows), bf16),
            pltpu.VMEM((HEADS, CHUNK * rows, NOPE + ROPE), bf16),
            pltpu.VMEM((HEADS, VDIM + 16, CHUNK * rows), bf16),
            pltpu.VMEM((HEADS, NY, VDIM + 16, rows), f32),
            pltpu.VMEM((HEADS, NY, 8, rows), f32),
        ),
        1,
    )(jnp.stack([z, y]).astype(jnp.int32), *held, gathered, wq, wk, gq, gk, cosine, sine)
    merged = lax.all_to_all(parts, "sp_1", 0, 0, tiled=True)
    partial = call(project_kernel, shapes((rows, conv_project.shape[1]), bf16), 2 * 256 * 256 * 2048)(
        merged, outer, gated, rim, conv_taps, conv_project, attend_project
    )
    share = rows // groups
    arrived = lax.all_to_all(
        partial.reshape(groups, share, -1), "tp", split_axis=0, concat_axis=0, tiled=True
    )
    return arrived.astype(f32).sum(axis=0).astype(bf16)


def solution(mesh):
    split = Mesh(mesh.devices.reshape(NZ, NY, mesh.shape["tp"]), ("sp_0", "sp_1", "tp"))
    in_specs = (
        P(SP, "tp"),
        P(None, "tp"),
        P(None, "tp"),
        P(None, "tp"),
        P(None, "tp"),
        P(None, "tp"),
        P(None, "tp"),
        P(),
        P(),
        P(),
        P(None, "tp"),
        P(None, "tp"),
        P("tp", None),
        P("tp", None),
    )
    out_specs = P(SP_TP, None)
    return jax.shard_map(local, mesh=split, in_specs=in_specs, out_specs=out_specs, check_vma=False)
```
